32 devices in a mesh: ep: 8 (over z, x), tp: 4 (over y, core).
Axes of the slice: x: 2, y: 2, z: 4, core: 2. Of those that a mesh axis runs over, the one named last changes fastest.
Arguments:
- query_rows: bfloat16 [3072, 1024], P('ep', 'tp'), may hold values from -8 to 8
- key_rows: bfloat16 [3072, 256], P('ep'), may hold values from -8 to 8
- value_rows: bfloat16 [3072, 256], P('ep'), may hold values from -6 to 6
- query_gain: float32 [64], replicated, may hold values from 0.3 to 6
- key_gain: float32 [64], replicated, may hold values from 0.3 to 6
- out_weight: bfloat16 [1024, 2048], P('tp'), may hold values from -0.1875 to 0.1875
- mixer_gain: float32 [2048], replicated, may hold values from 0.1 to 1.9
- expert_input: bfloat16 [2048, 2048], P('ep'), may hold values from -6 to 6
- expert_ids: int32 [2048, 2], P('ep'), may hold values from 0 to 7, all different within a row; in each aligned block of 256 rows (0 to 255, 256 to 511, ...) at most 96 rows name the same one
- gate_score: float32 [2048, 2], P('ep'), may hold values from 0.05 to 1
- expert_gain: float32 [2048], replicated, may hold values from 0.1 to 1.9
- gate_weight: bfloat16 [8, 2048, 4096], P('ep', None, 'tp'), may hold values from -0.125 to 0.125
- up_weight: bfloat16 [8, 2048, 4096], P('ep', None, 'tp'), may hold values from -0.125 to 0.125
- down_weight: bfloat16 [8, 4096, 2048], P('ep', 'tp'), may hold values from -0.09375 to 0.09375
- shared_gate: bfloat16 [2048, 2048], P(None, 'tp'), may hold values from -0.125 to 0.125
- shared_up: bfloat16 [2048, 2048], P(None, 'tp'), may hold values from -0.125 to 0.125
- shared_down: bfloat16 [2048, 2048], P('tp'), may hold values from -0.125 to 0.125
Outputs:
- mixer_out: bfloat16 [3072, 2048], P('ep')
- expert_out: bfloat16 [2048, 2048], P('ep', 'tp')
The draws below stay inside these ranges and needn't reach their ends.
Inputs may be any that keep to these rules, and one draw needn't show every extreme that they name: `expert_ids`: each row names 2 different experts. In each aligned block of 256 rows (the rows of one device) no expert is named by more than 96 rows, a bound that some block reaches.
All inputs are finite; a program needn't handle non-finite values.
Results may differ from the reference program's by a relative error of at most 0.02.
The reference program's roundings to bfloat16 on the way count: a program that leaves them out, or rounds other values in their place, can miss the bound.
Values may be sent and summed in bfloat16 or wider, within the bound.
A program may use at most 128 MiB of HBM per device.

```python
import math
import jax
import jax.numpy as jnp
import numpy as np
from jax import lax

D = 2048
HEADS = 16
KV_HEADS = 4
HEAD_DIM = 64
GRID_W = 64
EXPERT_DIM = 4096
SHARED_DIM = 2048
TOP = 2
RA = 384
RB = 256
TA = 3072
TB = 2048
EXPERTS = 8
CAP = 96
N_EP = 8
N_TP = 4


def draw_query_rows(key, part):
    drawn = jax.random.normal(jax.random.fold_in(key, 11), (TA, HEADS * HEAD_DIM), jnp.float32)
    drawn = jnp.clip(drawn, -6.0, 6.0)
    return drawn.astype(jnp.bfloat16)


def draw_key_rows(key, part):
    drawn = jax.random.normal(jax.random.fold_in(key, 12), (TA, KV_HEADS * HEAD_DIM), jnp.float32)
    drawn = jnp.clip(drawn, -6.0, 6.0)
    return drawn.astype(jnp.bfloat16)


def gain_draw(key, salt):
    drawn = 1.0 + 0.18 * jax.random.normal(jax.random.fold_in(key, salt), (HEAD_DIM,), jnp.float32)
    drawn = jnp.clip(drawn, 0.3, 1.7)
    return drawn.astype(jnp.float32)


def draw_query_gain(key, part):
    return gain_draw(key, 21)


def draw_key_gain(key, part):
    return gain_draw(key, 22)


def shard_levels(key, shape, cuts, low, top_value):
    level, own = 1.0, jax.random.fold_in(key, 6)
    for dim, parts in cuts:
        heights = jnp.exp(jax.random.uniform(jax.random.fold_in(own, dim), (parts,), jnp.float32, low / len(cuts), top_value / len(cuts)))
        level = level * jnp.repeat(heights, shape[dim] // parts).reshape([-1 if axis == dim else 1 for axis in range(len(shape))])
    return level


def assign_block(rng, own, number, rows, count, top, limit, lean):
    sequence = jax.random.permutation(rng, count)
    heavy_load, ordinary = load_shares(count, rows * top, limit, lean, True), load_shares(count, rows * top, limit, lean, False)
    places = jnp.arange(count)

    def named(tallies, rotation):
        used = int((tallies > 0).sum())
        fixed = max(1, used // 4)
        moved = fixed + (places - fixed + rotation * (used - fixed)) % max(1, count - fixed)
        return jnp.zeros((count,), jnp.int32).at[sequence[jnp.where(places < fixed, places, moved)]].set(jnp.asarray(tallies, jnp.int32))

    tallies = jnp.where(number % 4 == 0, named(heavy_load, number // 4), named(ordinary, number - number // 4 - 1))
    mixed = jax.random.permutation(jax.random.fold_in(own, 3), count)
    donor, taker = mixed[0:count // 2 * 2:2], mixed[1:count // 2 * 2:2]
    slack = jnp.minimum(tallies[donor] - 1, limit - tallies[taker]) // 2
    slack = jnp.where((donor == sequence[0]) | (taker == sequence[0]) | (tallies[taker] == 0), 0, jnp.maximum(slack, 0))
    moved = jax.random.randint(jax.random.fold_in(own, 4), (count // 2,), 0, 1 << 20) % (slack + 1)
    tallies = tallies.at[donor].add(-moved).at[taker].add(moved)
    items = jnp.searchsorted(jnp.cumsum(tallies), jnp.arange(rows * top), side="right").astype(jnp.int32)
    table = items.reshape(top, rows).T
    table = table[jax.random.permutation(jax.random.fold_in(own, 1), rows)]
    rotation = jax.random.randint(jax.random.fold_in(own, 2), (rows, 1), 0, top)
    return jnp.take_along_axis(table, (jnp.arange(top)[None, :] + rotation) % top, axis=1)


def load_shares(number_of, total, bound, lean, full):
    weights = [(1 << 20) // math.isqrt(standing ** lean) + 1 for standing in range(1, number_of + 1)]
    largest = bound if full else min(bound, max(-(-total // number_of), total * weights[0] // sum(weights)))
    least = 1 if total - largest >= number_of - 1 else 0
    holding, spare = [largest] + [least] * (number_of - 1), total - largest - least * (number_of - 1)
    while spare > 0:
        free = [i for i in range(1, number_of) if holding[i] < largest] or [i for i in range(1, number_of) if holding[i] < bound]
        pool, budget = sum([weights[i] for i in free]), spare
        for i in free:
            addition = min(bound - holding[i], max(1, budget * weights[i] // pool), spare)
            holding[i] = holding[i] + addition
            spare = spare - addition
    return np.array(holding)


def centred(own_key, extent, spread, most, pieces=(), kind=jnp.bfloat16):
    result = spread * jax.random.normal(own_key, extent, jnp.float32)
    if pieces:
        result = result * shard_levels(own_key, extent, pieces, -0.22, 0.18)
    return jnp.clip(result, -most, most).astype(kind)


def setup_inputs(seed: int = 0) -> dict:
    key_of = jax.random.split(jax.random.key(seed), 18)
    query_rows = draw_query_rows(jax.random.fold_in(key_of[17], 71), 0)
    key_rows = draw_key_rows(jax.random.fold_in(key_of[17], 71), 0)
    value_rows = centred(key_of[2], (TA, KV_HEADS * HEAD_DIM), 1.0, 6.0, ((0, 8),))
    query_gain = draw_query_gain(jax.random.fold_in(key_of[17], 71), 0)
    key_gain = draw_key_gain(jax.random.fold_in(key_of[17], 71), 0)
    out_weight = centred(key_of[5], (HEADS * HEAD_DIM, D), (HEADS * HEAD_DIM) ** -0.5, 0.1875, ((0, 4),))
    mixer_gain = jnp.clip(1.0 + 0.18 * jax.random.normal(key_of[6], (D,), jnp.float32), 0.1, 1.9)
    expert_input = centred(key_of[7], (TB, D), 1.0, 6.0, ((0, 8),))
    expert_ids_keys = jax.random.split(jax.random.fold_in(key_of[8], 1), TB // RB)
    expert_ids_turns = jax.random.permutation(jax.random.fold_in(key_of[8], 3), TB // RB)
    expert_ids = jax.vmap(lambda own, number: assign_block(jax.random.fold_in(key_of[8], 2), own, number, RB, EXPERTS, TOP, CAP, 2))(expert_ids_keys, expert_ids_turns).reshape((TB, TOP))
    gate_score = jnp.clip(jnp.exp(math.log(1.0) - 2.9957323 * jax.random.uniform(key_of[9], (TB, TOP), jnp.float32) ** shard_levels(key_of[9], (TB, TOP), ((0, 8),), -0.2, 0.2)), 0.05, 1.0)
    expert_gain = jnp.clip(1.0 + 0.18 * jax.random.normal(key_of[10], (D,), jnp.float32), 0.1, 1.9)
    gate_weight = centred(key_of[11], (EXPERTS, D, EXPERT_DIM), D ** -0.5, 0.125, ((0, 8), (2, 4)))
    up_weight = centred(key_of[12], (EXPERTS, D, EXPERT_DIM), D ** -0.5, 0.125, ((0, 8), (2, 4)))
    down_weight = centred(key_of[13], (EXPERTS, EXPERT_DIM, D), EXPERT_DIM ** -0.5, 0.09375, ((0, 8), (1, 4)))
    shared_gate = centred(key_of[14], (D, SHARED_DIM), D ** -0.5, 0.125, ((1, 4),))
    shared_up = centred(key_of[15], (D, SHARED_DIM), D ** -0.5, 0.125, ((1, 4),))
    shared_down = centred(key_of[16], (SHARED_DIM, D), SHARED_DIM ** -0.5, 0.125, ((0, 4),))
    return {"query_rows": query_rows, "key_rows": key_rows, "value_rows": value_rows, "query_gain": query_gain, "key_gain": key_gain, "out_weight": out_weight, "mixer_gain": mixer_gain, "expert_input": expert_input, "expert_ids": expert_ids, "gate_score": gate_score, "expert_gain": expert_gain, "gate_weight": gate_weight, "up_weight": up_weight, "down_weight": down_weight, "shared_gate": shared_gate, "shared_up": shared_up, "shared_down": shared_down}


EPSILON = 1e-06
ROUTED_SCALE = 2.5

def rotary_angles(position):
    grid_row = (position // GRID_W).astype(jnp.float32)
    grid_col = (position % GRID_W).astype(jnp.float32)
    quarter = HEAD_DIM // 4
    inverse = 10000.0 ** (-jnp.arange(quarter, dtype=jnp.float32) / quarter)
    return jnp.concatenate([grid_row[:, None] * inverse, grid_col[:, None] * inverse], axis=1)

def normalize_rotate(heads_in, gain_vector, angles):
    widened = heads_in.astype(jnp.float32)
    scaled = widened * lax.rsqrt(lax.optimization_barrier(jnp.mean(widened * widened, axis=-1, keepdims=True)) + EPSILON)
    scaled = scaled * gain_vector.astype(jnp.float32)
    half_dim = scaled.shape[-1] // 2
    front_half = scaled[..., :half_dim]
    back_half = scaled[..., half_dim:]
    cosine_table = jnp.cos(angles)[:, None, :]
    sine_table = jnp.sin(angles)[:, None, :]
    turned = jnp.concatenate([front_half * cosine_table - back_half * sine_table, front_half * sine_table + back_half * cosine_table], axis=-1)
    return turned.astype(jnp.bfloat16)

def swiglu(rows_in, gate_matrix, up_matrix):
    gate_value = jnp.dot(rows_in, gate_matrix, preferred_element_type=jnp.float32)
    up_value = jnp.dot(rows_in, up_matrix, preferred_element_type=jnp.float32)
    return (jax.nn.silu(gate_value) * up_value).astype(jnp.bfloat16)

def lane_sum(hidden, down_matrix):
    group_units = hidden.shape[1] // N_TP

    def add_group(carry, group_index):
        part_hidden = lax.dynamic_slice_in_dim(hidden, group_index * group_units, group_units, 1)
        part_down = lax.dynamic_slice_in_dim(down_matrix, group_index * group_units, group_units, 0)
        partial_value = jnp.dot(part_hidden, part_down, preferred_element_type=jnp.float32).astype(jnp.bfloat16)
        return (carry + lax.optimization_barrier(partial_value).astype(jnp.float32), None)
    start_total = jnp.zeros((hidden.shape[0], down_matrix.shape[1]), jnp.float32)
    total, unused = lax.scan(add_group, start_total, jnp.arange(N_TP, dtype=jnp.int32))
    return total

def fill_slots(empty_table, slot_rows, row_numbers):
    return empty_table.at[slot_rows].set(row_numbers)

def reference(query_rows, key_rows, value_rows, query_gain, key_gain, out_weight, mixer_gain, expert_input, expert_ids, gate_score, expert_gain, gate_weight, up_weight, down_weight, shared_gate, shared_up, shared_down):
    group = HEADS // KV_HEADS
    angles = rotary_angles(jnp.arange(TA, dtype=jnp.int32))
    query_rot = normalize_rotate(query_rows.reshape(TA, HEADS, HEAD_DIM), query_gain, angles)
    key_rot = normalize_rotate(key_rows.reshape(TA, KV_HEADS, HEAD_DIM), key_gain, angles)
    value_heads = value_rows.reshape(TA, KV_HEADS, HEAD_DIM)
    scale_factor = HEAD_DIM ** (-0.5)
    block_count = TA // RA

    def one_head(head_index):
        kv_index = head_index // group
        head_keys = lax.dynamic_index_in_dim(key_rot, kv_index, 1, keepdims=False)
        head_values = lax.dynamic_index_in_dim(value_heads, kv_index, 1, keepdims=False)
        head_queries = lax.dynamic_index_in_dim(query_rot, head_index, 1, keepdims=False)

        def one_block(query_block):
            scores = jnp.dot(query_block, head_keys.T, preferred_element_type=jnp.float32) * scale_factor
            row_peak = lax.optimization_barrier(jnp.max(scores, axis=1, keepdims=True))
            exponent = jnp.exp(scores - row_peak)
            row_total = lax.optimization_barrier(jnp.sum(exponent, axis=1, keepdims=True))
            weighted = jnp.dot(exponent.astype(jnp.bfloat16), head_values, preferred_element_type=jnp.float32)
            return (weighted / row_total).astype(jnp.bfloat16)
        return lax.map(one_block, head_queries.reshape(block_count, RA, HEAD_DIM)).reshape(TA, HEAD_DIM)
    attended = lax.map(one_head, jnp.arange(HEADS, dtype=jnp.int32))
    lane_heads = HEADS // N_TP
    attended_lanes = attended.reshape(N_TP, lane_heads, TA, HEAD_DIM)
    weight_lanes = out_weight.reshape(N_TP, lane_heads, HEAD_DIM, D)

    def add_lane(carry, packed):
        lane_attended, lane_weight = packed
        partial_value = jnp.einsum('hqd,hde->qe', lane_attended.astype(jnp.float32), lane_weight.astype(jnp.float32))
        rounded = lax.optimization_barrier(partial_value.astype(jnp.bfloat16))
        return (carry + rounded.astype(jnp.float32), None)
    mixer_sum, unused = lax.scan(add_lane, jnp.zeros((TA, D), jnp.float32), (attended_lanes, weight_lanes))
    mixer_scale = lax.rsqrt(lax.optimization_barrier(jnp.mean(mixer_sum * mixer_sum, axis=1, keepdims=True)) + EPSILON)
    mixer_out = (mixer_sum * mixer_scale * mixer_gain.astype(jnp.float32)).astype(jnp.bfloat16)
    widened = expert_input.astype(jnp.float32)
    normed = (widened * lax.rsqrt(lax.optimization_barrier(jnp.mean(widened * widened, axis=1, keepdims=True)) + EPSILON) * expert_gain.astype(jnp.float32)).astype(jnp.bfloat16)
    route_weight = gate_score / lax.optimization_barrier(jnp.sum(gate_score, axis=1, keepdims=True)) * ROUTED_SCALE
    pair_ids = expert_ids.reshape(N_EP, RB * TOP)
    onehot = (pair_ids[:, :, None] == jnp.arange(EXPERTS, dtype=jnp.int32)).astype(jnp.int32)
    ranks = lax.optimization_barrier(jnp.sum((jnp.cumsum(onehot, axis=1, dtype=jnp.int32) - 1) * onehot, axis=2, dtype=jnp.int32))
    slot_index = (pair_ids * CAP + ranks).astype(jnp.int32)
    row_numbers = (jnp.arange(N_EP, dtype=jnp.int32)[:, None] * RB + jnp.arange(RB * TOP, dtype=jnp.int32)[None, :] // TOP).astype(jnp.int32)
    sources = jnp.full((N_EP, EXPERTS * CAP), -1, jnp.int32)
    sources = jax.vmap(fill_slots)(sources, slot_index, row_numbers)
    expert_sources = sources.reshape(N_EP, EXPERTS, CAP).transpose(1, 0, 2).reshape(EXPERTS, N_EP * CAP)

    def one_expert(packed):
        source_rows, gate_matrix, up_matrix, down_matrix = packed
        filled = (source_rows >= 0)[:, None]
        picked = jnp.where(filled, normed[jnp.maximum(source_rows, 0)], jnp.zeros((), jnp.bfloat16))
        hidden = swiglu(picked, gate_matrix, up_matrix)
        return lane_sum(hidden, down_matrix).astype(jnp.bfloat16)
    expert_result = lax.map(one_expert, (expert_sources, gate_weight, up_weight, down_weight))
    flat_result = expert_result.reshape(EXPERTS * N_EP * CAP, D)
    block_of = (jnp.arange(TB, dtype=jnp.int32) // RB)[:, None]
    result_index = (expert_ids * (N_EP * CAP) + block_of * CAP + ranks.reshape(TB, TOP)).astype(jnp.int32)
    picked_results = flat_result[result_index]
    routed = lax.optimization_barrier(jnp.sum(picked_results.astype(jnp.float32) * route_weight[:, :, None], axis=1))
    shared_hidden = swiglu(normed, shared_gate, shared_up)
    shared_sum = lane_sum(shared_hidden, shared_down)
    expert_out = (routed + shared_sum).astype(jnp.bfloat16)
    return (mixer_out, expert_out)
```

```python
import functools

import jax
import jax.numpy as jnp
from jax import lax
from jax.experimental import pallas as pl
from jax.experimental.pallas import tpu as pltpu
from jax.sharding import PartitionSpec as P

HEADS = 16
KV_HEADS = 4
HEAD_DIM = 64
GRID_W = 64

EPSILON = 1e-06
ROUTED_SCALE = 2.5
F32 = jnp.float32
BF16 = jnp.bfloat16
MESH = pl.DeviceIdType.MESH


def rotary_angles(position):
    grid_row = (position // GRID_W).astype(F32)
    grid_col = (position % GRID_W).astype(F32)
    quarter = HEAD_DIM // 4
    inverse = 10000.0 ** (-jnp.arange(quarter, dtype=F32) / quarter)
    return jnp.concatenate([grid_row[:, None] * inverse, grid_col[:, None] * inverse], axis=1)


def normalize_rotate(heads_in, gain_vector, angles):
    widened = heads_in.astype(F32)
    scaled = widened * lax.rsqrt(jnp.mean(widened * widened, axis=-1, keepdims=True) + EPSILON)
    scaled = scaled * gain_vector
    half_dim = scaled.shape[-1] // 2
    front_half = scaled[..., :half_dim]
    back_half = scaled[..., half_dim:]
    cosine_table = jnp.cos(angles)[:, None, :]
    sine_table = jnp.sin(angles)[:, None, :]
    turned = jnp.concatenate(
        [
            front_half * cosine_table - back_half * sine_table,
            front_half * sine_table + back_half * cosine_table,
        ],
        axis=-1,
    )
    return turned.astype(BF16)


def silu(v):
    return v / (1.0 + jnp.exp(-v))


def dot(a, b):
    return jnp.dot(a, b, preferred_element_type=F32)


def fused_kernel(
    sizes,
    kv_in, out_in, q_in, normed_in, pick_in, gain_in,
    sg_hbm, su_hbm, sd_hbm, ow_hbm, wg_hbm, wu_hbm, wd_hbm,
    mixer_ref, expert_ref,
    sg, su, sd, ow, wg, wu, wd,
    kv, att, mp, mrecv, msum, my, mo, xh, hid, po, rp, tt, ret,
    sho, shs, shr, cf, cb, cr,
    w_sem, kv_s, kv_r, d_s, d_r, f_s, f_r, sh_sem, mp_sem, my_s, my_r, mo_sem,
    p_s, p_r, r_s, r_r, c_s, c_r,
):
    n, tp_n, ny, heads, cp, lc = sizes
    me = lax.axis_index("ep")
    tp = lax.axis_index("tp")
    core = tp % 2
    y = tp // 2
    mate = tp + 1 - 2 * core
    other = 1 - core
    ra = kv_in.shape[0]
    half = ra // 2

    def send(src, dst, ssem, rsem, ep=None, t=None):
        return pltpu.make_async_remote_copy(
            src_ref=src, dst_ref=dst, send_sem=ssem, recv_sem=rsem,
            device_id=(me if ep is None else ep, tp if t is None else t), device_id_type=MESH,
        )

    def rows(block, size):
        return pl.ds(pl.multiple_of(block * size, size), size)

    def each(lo, hi, fn):
        def step(i, c):
            fn(i)
            return c
        lax.fori_loop(lo, hi, step, 0)

    weights = [
        pltpu.make_async_copy(a, b, w_sem.at[i])
        for i, (a, b) in enumerate(
            ((sg_hbm, sg), (su_hbm, su), (sd_hbm, sd), (ow_hbm, ow), (wg_hbm, wg), (wu_hbm, wu), (wd_hbm, wd))
        )
    ]
    for copy in weights:
        copy.start()

    barrier = pltpu.get_barrier_semaphore()

    def greet(s):
        pl.semaphore_signal(barrier, inc=1, device_id=((me + s) % n, tp), device_id_type=MESH)

    def greet_y(s):
        pl.semaphore_signal(barrier, inc=1, device_id=(me, (tp + 2 * s) % tp_n), device_id_type=MESH)

    each(1, n, greet)
    each(1, ny, greet_y)
    pl.semaphore_signal(barrier, inc=1, device_id=(me, mate), device_id_type=MESH)
    pl.semaphore_wait(barrier, n - 1 + ny - 1 + 1)

    def kv_copy(src, to):
        return send(kv_in, kv.at[rows(src, ra)], kv_s.at[to], kv_r.at[src], ep=to)

    def d_copy(src, to):
        return send(out_in.at[rows(to, cp)], xh.at[core, rows(src, cp)], d_s.at[to], d_r.at[src], ep=to)

    each(1, n, lambda s: kv_copy(me, (me + s) % n).start())
    each(1, n, lambda s: d_copy(me, (me + s) % n).start())

    def own_forward():
        return send(out_in.at[rows(me, cp)], xh.at[core, rows(me, cp)], f_s.at[me], f_r.at[me], t=mate)

    def forward(src):
        return send(xh.at[core, rows(src, cp)], xh.at[core, rows(src, cp)], f_s.at[src], f_r.at[src], t=mate)

    own_forward().start()
    kv[rows(me, ra), :] = kv_in[...]
    xh[core, rows(me, cp), :] = out_in[rows(me, cp), :]

    for i in range(3):
        weights[i].wait()
    normed = normed_in[...]
    sh_hidden = (silu(dot(normed, sg[...])) * dot(normed, su[...])).astype(BF16)

    def cols(tile):
        return pl.ds(pl.multiple_of(tile * lc, lc), lc)

    for q in range(ny):
        sho[q] = dot(sh_hidden, sd[:, cols(2 * q + other)]).astype(BF16)
    sh_copy = send(sho, shr, sh_sem.at[0], sh_sem.at[1], t=mate)
    sh_copy.start()
    for q in range(ny):
        shs[q] = dot(sh_hidden, sd[:, cols(2 * q + core)]).astype(BF16)

    each(1, n, lambda s: kv_copy((me + n - s) % n, me).wait_recv())
    total = kv.shape[0]
    bq = max(16, min(ra, 128 * 3072 // total // 16 * 16))
    while ra % bq:
        bq -= 16
    per_head = ra // bq

    def attend(i):
        block = q_in[pl.ds(pl.multiple_of(i * bq, bq), bq), :]
        scores = lax.dot_general(block, kv[...], (((1,), (1,)), ((), ())), preferred_element_type=F32)
        peak = jnp.max(scores, axis=1, keepdims=True)
        exponent = jnp.exp(scores - peak)
        row_total = jnp.sum(exponent, axis=1, keepdims=True)
        weighted = dot(exponent.astype(BF16), kv[...])
        att[pl.ds(pl.multiple_of((i % per_head) * bq, bq), bq),
            pl.ds(pl.multiple_of((i // per_head) * 128, 128), 128)] = (weighted / row_total).astype(BF16)

    steps = heads * per_head
    pair = 2 if steps % 2 == 0 else 1

    def attend_pair(i):
        for j in range(pair):
            attend(i * pair + j)

    each(0, steps // pair, attend_pair)

    def pass_on(s):
        src = (me + n - s) % n
        d_copy(src, me).wait_recv()
        forward(src).start()

    each(1, n, pass_on)

    weights[3].wait()
    width = mp.shape[1]
    tile = min(512, width)

    def project(t):
        at = pl.ds(pl.multiple_of(t * tile, tile), tile)
        mp[:, at] = dot(att[...], ow[:, at]).astype(BF16)

    each(0, width // tile, project)
    mp_copy = send(mp.at[rows(other, half)], mrecv, mp_sem.at[0], mp_sem.at[1], t=mate)
    mp_copy.start()

    weights[4].wait()
    weights[5].wait()
    each(0, n, lambda s: send(
        xh.at[other, rows(s, cp)], xh.at[other, rows(s, cp)], f_s.at[s], f_r.at[s], t=mate).wait_recv())
    depth = xh.shape[2]
    ft = min(256, hid.shape[1])

    def gate_up(t):
        at = pl.ds(pl.multiple_of(t * ft, ft), ft)
        gate = dot(xh[0], wg[0:depth, at]) + dot(xh[1], wg[depth:, at])
        up = dot(xh[0], wu[0:depth, at]) + dot(xh[1], wu[depth:, at])
        hid[:, at] = (silu(gate) * up).astype(BF16)

    each(0, 1, gate_up)
    mp_copy.wait_recv()
    msum[...] = (mp[rows(core, half), :].astype(F32) + mrecv[...].astype(F32)).astype(BF16)

    def my_copy(src, to):
        return send(msum, my.at[src], my_s.at[to], my_r.at[src], t=2 * to + core)

    each(1, ny, lambda s: my_copy(y, (y + s) % ny).start())
    my[y] = msum[...]
    each(1, hid.shape[1] // ft, gate_up)

    weights[6].wait()

    def p_copy(q):
        return send(po.at[q], rp.at[q], p_s.at[q], p_r.at[q], t=mate)

    def down_other(q):
        po[q] = dot(hid[...], wd[:, cols(2 * q + other)]).astype(BF16)
        p_copy(q).start()

    each(0, ny, down_other)

    def r_copy(q, src, to):
        return send(tt.at[q, rows(to, cp)], ret.at[q, rows(src, cp)], r_s.at[q, to], r_r.at[q, src], ep=to)

    def down_own(q):
        own = dot(hid[...], wd[:, cols(2 * q + core)]).astype(BF16).astype(F32)
        p_copy(q).wait_recv()
        tt[q] = (own + rp[q].astype(F32)).astype(BF16)
        each(1, n, lambda s: r_copy(q, me, (me + s) % n).start())
        ret[q, rows(me, cp), :] = tt[q, rows(me, cp), :]

    def down_step(s):
        down_own((y + s) % ny)

    each(1, ny + 1, down_step)

    each(1, ny, lambda s: my_copy((y + s) % ny, y).wait_recv())
    mixed = my[0].astype(F32)
    for j in range(1, ny):
        mixed = mixed + my[j].astype(F32)
    scale = lax.rsqrt(jnp.mean(mixed * mixed, axis=1, keepdims=True) + EPSILON)
    msum_out = (mixed * scale * gain_in[...]).astype(BF16)
    mixer_ref[rows(core, half), :] = msum_out
    mp_copy.wait_send()
    mp[rows(core, half), :] = msum_out
    mo_copy = send(mp.at[rows(core, half)], mo, mo_sem.at[0], mo_sem.at[1], t=mate)
    mo_copy.start()
    mo_copy.wait_recv()
    mixer_ref[rows(other, half), :] = mo[...]

    sh_copy.wait_recv()

    def combine(q):
        each(1, n, lambda s: r_copy(q, (me + n - s) % n, me).wait_recv())
        routed = dot(pick_in[0], ret[q]) + dot(pick_in[1], ret[q])
        return routed + shs[q].astype(F32) + shr[q].astype(F32)

    def c_copy(src, to):
        return send(cb.at[to], cr.at[src], c_s.at[to], c_r.at[src], t=2 * to + core)

    def combine_far(s):
        q = (y + s) % ny
        cb[q] = combine(q).astype(BF16)
        c_copy(y, q).start()

    each(1, ny, combine_far)
    cf[...] = combine(y)

    def collect(s):
        src = (y + s) % ny
        c_copy(src, y).wait_recv()
        cf[...] += cr[src].astype(F32)

    each(1, ny, collect)
    expert_ref[...] = cf[...].astype(BF16)

    def drain(s):
        to = (me + s) % n
        kv_copy(me, to).wait_send()
        d_copy(me, to).wait_send()
        forward((me + s) % n).wait_send()
        each(0, ny, lambda q: r_copy(q, me, to).wait_send())

    each(1, n, drain)
    own_forward().wait_send()
    sh_copy.wait_send()
    mo_copy.wait_send()
    each(0, ny, lambda q: p_copy(q).wait_send())

    def drain_y(s):
        to = (y + s) % ny
        my_copy(y, to).wait_send()
        c_copy(y, to).wait_send()

    each(1, ny, drain_y)


def body(
    query_rows, key_rows, value_rows, query_gain, key_gain, out_weight, mixer_gain,
    expert_input, expert_ids, gate_score, expert_gain,
    gate_weight, up_weight, down_weight, shared_gate, shared_up, shared_down,
):
    n = lax.axis_size("ep")
    tp_n = lax.axis_size("tp")
    ny = tp_n // 2
    me = lax.axis_index("ep")
    tp = lax.axis_index("tp")
    ra = query_rows.shape[0]
    heads = query_rows.shape[1] // HEAD_DIM
    first_kv = tp * heads // (HEADS // KV_HEADS)
    angles = rotary_angles(me * ra + jnp.arange(ra, dtype=jnp.int32))
    query_rot = normalize_rotate(query_rows.reshape(ra, heads, HEAD_DIM), query_gain, angles)
    query_rot = query_rot * BF16(HEAD_DIM ** (-0.5))
    q_in = jnp.pad(query_rot.transpose(1, 0, 2), ((0, 0), (0, 0), (0, HEAD_DIM))).reshape(heads * ra, 2 * HEAD_DIM)
    key_cols = lax.dynamic_slice_in_dim(key_rows, first_kv * HEAD_DIM, HEAD_DIM, 1)
    value_cols = lax.dynamic_slice_in_dim(value_rows, first_kv * HEAD_DIM, HEAD_DIM, 1)
    key_rot = normalize_rotate(key_cols.reshape(ra, 1, HEAD_DIM), key_gain, angles)
    kv_in = jnp.concatenate([key_rot.reshape(ra, HEAD_DIM), value_cols], axis=1)
    width = out_weight.shape[1]
    ow_pad = jnp.pad(out_weight.reshape(heads, HEAD_DIM, width), ((0, 0), (HEAD_DIM, 0), (0, 0)))
    ow_pad = ow_pad.reshape(heads * 2 * HEAD_DIM, width)
    rb, top = expert_ids.shape
    experts = n * gate_weight.shape[0]
    cap = 3 * rb * top // (2 * experts)
    cp = -(-cap // 16) * 16
    model = expert_input.shape[1]
    lc = model // tp_n
    widened = expert_input.astype(F32)
    normed = (
        widened * lax.rsqrt(jnp.mean(widened * widened, axis=1, keepdims=True) + EPSILON) * expert_gain
    ).astype(BF16)
    route_weight = gate_score / jnp.sum(gate_score, axis=1, keepdims=True) * ROUTED_SCALE
    named = expert_ids[:, :, None] == jnp.arange(experts, dtype=jnp.int32)
    member = jnp.any(named, axis=1)
    row_weight = jnp.sum(jnp.where(named, route_weight[:, :, None], 0.0), axis=1)
    before = jnp.tril(jnp.ones((rb, rb), BF16), -1)
    rank = dot(before, member.astype(BF16)).astype(jnp.int32)
    slot = jnp.where(member, rank, -1)
    chosen = slot[:, :, None] == jnp.arange(cp, dtype=jnp.int32)
    weight = jnp.where(chosen, row_weight[:, :, None], 0.0).reshape(rb, experts * cp)
    high = weight.astype(BF16)
    low = (weight - high.astype(F32)).astype(BF16)
    pick = jnp.stack([high, low])
    choose = chosen.astype(BF16).reshape(rb, experts * cp)
    own_cols = lax.dynamic_slice_in_dim(normed, (tp % 2) * (model // 2), model // 2, 1)
    outgoing = lax.dot_general(
        choose, own_cols, (((0,), (0,)), ((), ())), preferred_element_type=F32
    ).astype(BF16)

    slots = n * cp
    hidden = gate_weight.shape[2]
    sh = shared_gate.shape[1]
    vm = pltpu.VMEM
    dma = pltpu.SemaphoreType.DMA
    half = ra // 2
    vspec = pl.BlockSpec(memory_space=pltpu.VMEM)
    hspec = pl.BlockSpec(memory_space=pl.ANY)
    sizes = (n, tp_n, ny, heads, cp, lc)
    return pl.pallas_call(
        functools.partial(fused_kernel, sizes),
        out_shape=(
            jax.ShapeDtypeStruct((ra, width), BF16),
            jax.ShapeDtypeStruct((rb, lc), BF16),
        ),
        in_specs=[vspec] * 6 + [hspec] * 7,
        out_specs=(vspec, vspec),
        scratch_shapes=[
            vm((model, sh), BF16), vm((model, sh), BF16), vm((sh, model), BF16),
            vm((heads * 2 * HEAD_DIM, width), BF16),
            vm((model, hidden), BF16), vm((model, hidden), BF16), vm((hidden, model), BF16),
            vm((n * ra, 2 * HEAD_DIM), BF16),
            vm((ra, heads * 2 * HEAD_DIM), BF16),
            vm((ra, width), BF16), vm((half, width), BF16), vm((half, width), BF16),
            vm((ny, half, width), BF16), vm((half, width), BF16),
            vm((2, slots, model // 2), BF16), vm((slots, hidden), BF16),
            vm((ny, slots, lc), BF16), vm((ny, slots, lc), BF16),
            vm((ny, slots, lc), BF16), vm((ny, slots, lc), BF16),
            vm((ny, rb, lc), BF16), vm((ny, rb, lc), BF16), vm((ny, rb, lc), BF16),
            vm((rb, lc), F32), vm((ny, rb, lc), BF16), vm((ny, rb, lc), BF16),
            dma((7,)), dma((n,)), dma((n,)), dma((n,)), dma((n,)), dma((n,)), dma((n,)),
            dma((2,)), dma((2,)), dma((ny,)), dma((ny,)), dma((2,)),
            dma((ny,)), dma((ny,)), dma((ny, n)), dma((ny, n)), dma((ny,)), dma((ny,)),
        ],
        compiler_params=pltpu.CompilerParams(
            collective_id=0, has_side_effects=True, vmem_limit_bytes=64 * 1024 * 1000
        ),
        name="fused_layer",
    )(
        kv_in, outgoing, q_in, normed, pick, mixer_gain.reshape(1, width),
        shared_gate, shared_up, shared_down, ow_pad,
        gate_weight[0], up_weight[0], down_weight[0],
    )


def solution(mesh):
    in_specs = (
        P("ep", "tp"), P("ep", None), P("ep", None), P(), P(), P("tp", None), P(),
        P("ep", None), P("ep", None), P("ep", None), P(),
        P("ep", None, "tp"), P("ep", None, "tp"), P("ep", "tp", None),
        P(None, "tp"), P(None, "tp"), P("tp", None),
    )
    out_specs = (P("ep", None), P("ep", "tp"))
    return jax.shard_map(body, mesh=mesh, in_specs=in_specs, out_specs=out_specs, check_vma=False)
```
